256 devices in a mesh: ep: 32 (over z, x), tp: 8 (over y, core).
Axes of the slice: x: 4, y: 4, z: 8, core: 2. Of those that a mesh axis runs over, the one named last changes fastest.
Arguments:
- tokens: bfloat16 [16384, 4096], P('ep', 'tp'), may hold values from -60 to 60
- routes: int32 [16384, 4], P('ep'), may hold values from 0 to 127, all different within a row; in each aligned block of 512 rows (0 to 511, 512 to 1023, ...) at most 32 rows name the same one
- route_weights: float32 [16384, 4], P('ep'), may hold values from 0.1 to 1
- pre_gain: float32 [4096], P('tp'), may hold values from 0.1 to 1.9
- expert_gate: bfloat16 [128, 4096, 512], P('ep', 'tp'), may hold values from -0.09375 to 0.09375
- expert_up: bfloat16 [128, 4096, 512], P('ep', 'tp'), may hold values from -0.09375 to 0.09375
- expert_down: bfloat16 [128, 512, 4096], P('ep', None, 'tp'), may hold values from -1 to 1
- shared_gate: bfloat16 [4096, 512], P('tp'), may hold values from -0.09375 to 0.09375
- shared_up: bfloat16 [4096, 512], P('tp'), may hold values from -0.09375 to 0.09375
- shared_down: bfloat16 [512, 4096], P(None, 'tp'), may hold values from -1 to 1
- post_gain: float32 [4096], P('tp'), may hold values from 0.1 to 1.9
Outputs:
- layer_out: bfloat16 [16384, 4096], P('ep', 'tp')
The draws below stay inside these ranges and needn't reach their ends.
Inputs may be any that keep to these rules, and one draw needn't show every extreme that they name: `routes`: each row names 4 different experts. Within each aligned block of 512 rows (the tokens of one index of ep) no expert is named more than 32 times, a bound that some block reaches.
All inputs are finite; a program needn't handle non-finite values.
Results may differ from the reference program's by a relative error of at most 0.022.
Values may be sent and summed in bfloat16 or wider, within the bound.
A program may use at most 128 MiB of HBM per device.

```python
import math
import jax
import jax.numpy as jnp
import numpy as np
from jax import lax

D = 4096
FF = 512
FS = 512
TOPK = 4
TOK_EP = 512
EXPERTS = 128
TOKENS = 16384
CAP = 32
N_EP = 32
N_TP = 8


def draw_tokens(key, part):
    key_base, key_rows, key_cols = jax.random.split(key, 3)
    ramp = 3.0 ** (jnp.arange(D, dtype=jnp.float32) / D)
    columns = ramp * jax.random.uniform(key_cols, (D,), jnp.float32, 0.5, 2.0)
    scales = jnp.exp(jax.random.uniform(key_rows, (TOKENS, 1), jnp.float32, -1.0, 1.0))
    base = jnp.clip(jax.random.normal(key_base, (TOKENS, D), jnp.float32), -6.0, 6.0)
    return jnp.clip(base * scales * columns, -60.0, 60.0).astype(jnp.bfloat16)


def ramped_weight(key, shape, fan_in):
    key_base, key_cols = jax.random.split(key)
    ramp = 3.0 ** (jnp.arange(D, dtype=jnp.float32) / D)
    columns = ramp * jax.random.uniform(key_cols, (D,), jnp.float32, 0.5, 2.0) / 2.0
    base = jnp.clip(jax.random.normal(key_base, shape, jnp.float32), -6.0, 6.0) * fan_in ** (-0.5)
    return jnp.clip(base * columns, -1.0, 1.0).astype(jnp.bfloat16)


def draw_expert_down(key, part):
    return ramped_weight(key, (EXPERTS, FF, D), FF)


def draw_shared_down(key, part):
    return ramped_weight(key, (FS, D), FS)


def steps_of(rng, dims, cuts, low, top_value):
    def one(position, shards_of):
        steps = jax.random.uniform(jax.random.fold_in(jax.random.fold_in(rng, 6), position), (shards_of,), jnp.float32, low / len(cuts), top_value / len(cuts))
        return jnp.repeat(jnp.exp(steps), dims[position] // shards_of).reshape((-1,) + (1,) * (len(dims) - position - 1))

    factor_of = one(*cuts[0])
    for cut in cuts[1:]:
        factor_of = factor_of * one(*cut)
    return factor_of


def routed_block(rng, own, number, rows, number_of, top, limit, slope):
    ranking = jax.random.permutation(rng, number_of)
    heavy_load, usual = shares(number_of, rows * top, limit, slope, True), shares(number_of, rows * top, limit, slope, False)
    places = jnp.arange(number_of)

    def named(sizes, offset_by):
        used = int((sizes > 0).sum())
        fixed = max(1, used // 4)
        moved = fixed + (places - fixed + offset_by * (used - fixed)) % max(1, number_of - fixed)
        return jnp.zeros((number_of,), jnp.int32).at[ranking[jnp.where(places < fixed, places, moved)]].set(jnp.asarray(sizes, jnp.int32))

    sizes = jnp.where(number % 4 == 0, named(heavy_load, number // 4), named(usual, number - number // 4 - 1))
    mixed = jax.random.permutation(jax.random.fold_in(own, 3), number_of)
    source_of, sink = mixed[0:number_of // 2 * 2:2], mixed[1:number_of // 2 * 2:2]
    slack = jnp.minimum(sizes[source_of] - 1, limit - sizes[sink]) // 2
    slack = jnp.where((source_of == ranking[0]) | (sink == ranking[0]) | (sizes[sink] == 0), 0, jnp.maximum(slack, 0))
    moved = jax.random.randint(jax.random.fold_in(own, 4), (number_of // 2,), 0, 1 << 20) % (slack + 1)
    sizes = sizes.at[source_of].add(-moved).at[sink].add(moved)
    labels = jnp.searchsorted(jnp.cumsum(sizes), jnp.arange(rows * top), side="right").astype(jnp.int32)
    table = labels.reshape(top, rows).T
    table = table[jax.random.permutation(jax.random.fold_in(own, 1), rows)]
    offset_by = jax.random.randint(jax.random.fold_in(own, 2), (rows, 1), 0, top)
    return jnp.take_along_axis(table, (jnp.arange(top)[None, :] + offset_by) % top, axis=1)


def shares(count, total, reach, lean, full):
    portions = [(1 << 20) // math.isqrt(grade ** lean) + 1 for grade in range(1, count + 1)]
    largest = reach if full else min(reach, max(-(-total // count), total * portions[0] // sum(portions)))
    least = 1 if total - largest >= count - 1 else 0
    counts, surplus = [largest] + [least] * (count - 1), total - largest - least * (count - 1)
    while surplus > 0:
        candidates = [i for i in range(1, count) if counts[i] < largest] or [i for i in range(1, count) if counts[i] < reach]
        mass, budget = sum([portions[i] for i in candidates]), surplus
        for i in candidates:
            extra = min(reach - counts[i], max(1, budget * portions[i] // mass), surplus)
            counts[i] = counts[i] + extra
            surplus = surplus - extra
    return np.array(counts)


def centred(rng, shape, width, reach, cuts=(), kind=jnp.bfloat16):
    gain = steps_of(rng, shape, cuts, -0.22, 0.18) if cuts else 1.0
    drawn = jax.random.normal(rng, shape, jnp.float32) * width * gain
    return jnp.minimum(jnp.maximum(drawn, -reach), reach).astype(kind)


def setup_inputs(seed: int = 0) -> dict:
    streams_of = jax.random.split(jax.random.key(seed), 12)
    tokens = draw_tokens(jax.random.fold_in(streams_of[11], 71), 0)
    routes_keys = jax.random.split(jax.random.fold_in(streams_of[1], 1), TOKENS // TOK_EP)
    routes_turns = jax.random.permutation(jax.random.fold_in(streams_of[1], 3), TOKENS // TOK_EP)
    routes = jax.vmap(lambda own, number: routed_block(jax.random.fold_in(streams_of[1], 2), own, number, TOK_EP, EXPERTS, TOPK, CAP, 2))(routes_keys, routes_turns).reshape((TOKENS, TOPK))
    route_weights = jnp.clip(jnp.exp(math.log(1.0) - 2.3025851 * jax.random.uniform(streams_of[2], (TOKENS, TOPK), jnp.float32) ** steps_of(streams_of[2], (TOKENS, TOPK), ((0, 32),), -0.2, 0.2)), 0.1, 1.0)
    pre_gain = jnp.clip(1.0 + 0.18 * jax.random.normal(streams_of[3], (D,), jnp.float32), 0.1, 1.9)
    expert_gate = centred(streams_of[4], (EXPERTS, D, FF), D ** -0.5, 0.09375, ((0, 32), (1, 8)))
    expert_up = centred(streams_of[5], (EXPERTS, D, FF), D ** -0.5, 0.09375, ((0, 32), (1, 8)))
    expert_down = draw_expert_down(jax.random.fold_in(streams_of[11], 71), 0)
    shared_gate = centred(streams_of[7], (D, FS), D ** -0.5, 0.09375, ((0, 8),))
    shared_up = centred(streams_of[8], (D, FS), D ** -0.5, 0.09375, ((0, 8),))
    shared_down = draw_shared_down(jax.random.fold_in(streams_of[11], 71), 0)
    post_gain = jnp.clip(1.0 + 0.18 * jax.random.normal(streams_of[10], (D,), jnp.float32), 0.1, 1.9)
    return {"tokens": tokens, "routes": routes, "route_weights": route_weights, "pre_gain": pre_gain, "expert_gate": expert_gate, "expert_up": expert_up, "expert_down": expert_down, "shared_gate": shared_gate, "shared_up": shared_up, "shared_down": shared_down, "post_gain": post_gain}


epsilon = 1e-06

def inverse_norm(values):
    return lax.rsqrt(lax.optimization_barrier(jnp.mean(values * values, axis=1)) + epsilon)

def blocked_product(inputs, weight):
    row_count = inputs.shape[0]
    out_width = weight.shape[1]
    pieces = inputs.reshape(row_count, N_TP, D // N_TP).astype(jnp.float32)
    blocks = weight.reshape(N_TP, D // N_TP, out_width).astype(jnp.float32)
    partial_value = jnp.einsum('rnd,ndf->nrf', pieces, blocks)
    rounded = lax.optimization_barrier(partial_value.astype(jnp.bfloat16))
    return lax.optimization_barrier(jnp.sum(rounded.astype(jnp.float32), axis=0))

def reference(tokens, routes, route_weights, pre_gain, expert_gate, expert_up, expert_down, shared_gate, shared_up, shared_down, post_gain):
    inputs = tokens.astype(jnp.float32)
    normed = (inputs * inverse_norm(inputs)[:, None] * pre_gain.astype(jnp.float32)).astype(jnp.bfloat16)
    per_block = TOK_EP * TOPK
    flat_ids = routes.reshape(N_EP, per_block).astype(jnp.int32)
    one_hot = (flat_ids[:, :, None] == jnp.arange(EXPERTS, dtype=jnp.int32)[None, None, :]).astype(jnp.int32)
    slots = lax.optimization_barrier(jnp.sum(jnp.cumsum(one_hot, axis=1) * one_hot, axis=2)) - 1
    sources = jnp.arange(N_EP, dtype=jnp.int32)[:, None]
    positions = (sources * CAP + slots).reshape(-1).astype(jnp.int32)
    token_index = (sources * TOK_EP + jnp.arange(per_block, dtype=jnp.int32)[None, :] // TOPK).reshape(-1).astype(jnp.int32)
    expert_index = flat_ids.reshape(-1)
    token_table = jnp.full((EXPERTS, N_EP * CAP), TOKENS, jnp.int32).at[expert_index, positions].set(token_index)
    weight_table = jnp.zeros((EXPERTS, N_EP * CAP), jnp.float32).at[expert_index, positions].set(route_weights.reshape(-1).astype(jnp.float32))

    def expert_step(totals, stacked):
        table_rows, table_weights, gate_weight, up_weight, down_weight = stacked
        arrived = jnp.take(normed, table_rows, axis=0, mode='fill', fill_value=0)
        gate_pre = blocked_product(arrived, gate_weight)
        up_pre = blocked_product(arrived, up_weight)
        hidden = (jax.nn.silu(gate_pre) * up_pre).astype(jnp.bfloat16)
        expert_out = jnp.dot(hidden, down_weight, preferred_element_type=jnp.float32).astype(jnp.bfloat16)
        totals = totals.at[table_rows].add(table_weights[:, None] * expert_out.astype(jnp.float32), mode='drop')
        return (totals, None)
    routed, _ = lax.scan(expert_step, jnp.zeros((TOKENS, D), jnp.float32), (token_table, weight_table, expert_gate, expert_up, expert_down))
    shared_gate_pre = blocked_product(normed, shared_gate)
    shared_up_pre = blocked_product(normed, shared_up)
    shared_hidden = (jax.nn.silu(shared_gate_pre) * shared_up_pre).astype(jnp.bfloat16)
    shared_out = jnp.dot(shared_hidden, shared_down, preferred_element_type=jnp.float32).astype(jnp.bfloat16)
    mixture = routed + shared_out.astype(jnp.float32)
    return (mixture * inverse_norm(mixture)[:, None] * post_gain.astype(jnp.float32)).astype(jnp.bfloat16)
```

```python
import functools

import jax
import jax.numpy as jnp
from jax import lax
from jax.experimental import pallas as pl
from jax.experimental.pallas import tpu as pltpu
from jax.sharding import PartitionSpec as P

MESH = pl.DeviceIdType.MESH
BF, F32 = jnp.bfloat16, jnp.float32
epsilon = 1e-06

NX, NC = 4, 2
CAP = 32

STAGES = ((0,), (1, 7), (2, 6), (3, 5), (4,), None)
SHARED = 5
OFFSET = (0, 64, 192, 320, 448, 512)
ROWS = 576

SCHEDULE = " ".join(
    (
        "A0 B0 C5 D5",
        "A1 B1 E5 C0",
        "D0 F5 A2 B2",
        "E0 C1 D1 A3",
        "B3 F0 G5 G0",
        "E1 C2 D2 A4",
        "B4 F1 G1 E2",
        "C4 D4 F2 C3",
        "D3 G2 E4 F4",
        "G4 E3 F3 G3",
        "Z4 Z3 Z2 Z1",
        "Z0",
    )
).split()


def kernel(
    nz,
    ny,
    features,
    schedule,
    tok_hbm,
    meta_in,
    gain,
    post,
    wg_hbm,
    wu_hbm,
    wd_hbm,
    sg_hbm,
    su_hbm,
    sd_hbm,
    out_ref,
    normed,
    wg,
    wu,
    wd,
    blocks,
    meta,
    inv,
    rows_out,
    rows_in,
    own_part,
    for_partner,
    from_partner,
    from_y,
    hid,
    returned,
    shared_out,
    z_in,
    part,
    mix,
    sums,
    send_sem,
    recv_sem,
    local_sem,
):
    ep, tp = lax.axis_index("ep"), lax.axis_index("tp")
    z, x = ep // NX, ep % NX
    y, c = tp // NC, tp % NC
    n_tok = normed.shape[0]
    half = n_tok // 2

    def device(dz=0, dx=0, dy=0, dc=0):
        return (
            (z + dz + nz) % nz * NX + (x + dx + NX) % NX,
            (y + dy + ny) % ny * NC + (c + dc) % NC,
        )

    used = [0, 0]
    sends, awaited = {}, {}

    def push(src, dst, to):
        i = used[0]
        used[0] += 1
        copy = pltpu.make_async_remote_copy(
            src_ref=src,
            dst_ref=dst,
            send_sem=send_sem.at[i],
            recv_sem=recv_sem.at[i],
            device_id=to,
            device_id_type=MESH,
        )
        copy.start()
        sends[id(copy)] = copy
        awaited[id(copy)] = copy
        return copy

    def got(copy):
        awaited.pop(id(copy)).wait_recv()

    def sent(copies):
        for copy in copies:
            sends.pop(id(copy)).wait_send()

    def load(src, dst):
        copy = pltpu.make_async_copy(src, dst, local_sem.at[used[1]])
        used[1] += 1
        copy.start()
        return copy

    token_load = load(tok_hbm, blocks.at[0])
    weight_loads = {
        "shared": [load(sg_hbm, wg.at[4]), load(su_hbm, wu.at[4])],
        "up": [load(wg_hbm, wg.at[pl.ds(0, 4)]), load(wu_hbm, wu.at[pl.ds(0, 4)])],
        "down": [load(sd_hbm, wd.at[4]), load(wd_hbm, wd.at[pl.ds(0, 4)])],
    }

    def need(name):
        for copy in weight_loads.pop(name, []):
            copy.wait()

    peers = [device(dz=1), device(dz=-1)]
    peers += [device(dx=dx) for dx in range(1, NX)]
    tp_steps = [(dy, dc) for dy in range(ny) for dc in range(NC)][1:]
    peers += [device(dy=dy, dc=dc) for dy, dc in tp_steps]
    barrier = pltpu.get_barrier_semaphore()
    for peer in peers:
        pl.semaphore_signal(barrier, inc=1, device_id=peer, device_id_type=MESH)

    def to_row(column):
        n = column.shape[0]
        same = lax.broadcasted_iota(jnp.int32, (n, n), 0) == lax.broadcasted_iota(
            jnp.int32, (n, n), 1
        )
        return jnp.sum(jnp.where(same, column, 0.0), axis=0, keepdims=True)

    def spread(row, width):
        high = row.astype(BF)
        rest = row - high.astype(F32)
        middle = rest.astype(BF)
        low = (rest - middle.astype(F32)).astype(BF)
        left = jnp.concatenate([high, middle, low, jnp.zeros((13, row.shape[1]), BF)], axis=0)
        column = lax.dot_general(
            left, jnp.ones((16, 128), BF), (((0,), (0,)), ((), ())), preferred_element_type=F32
        )
        return jnp.concatenate([column] * (width // 128), axis=1)

    def start_norm(values, which, cols):
        sums[which, 0, :, cols] = to_row(jnp.sum(values * values, axis=1, keepdims=True))
        return [
            push(
                sums.at[which, 0, :, cols],
                sums.at[which, i + 1, :, cols],
                device(dy=dy, dc=dc),
            )
            for i, (dy, dc) in enumerate(tp_steps)
        ]

    def end_norm(copies, which, cols):
        total = sums[which, 0, :, cols]
        for i, copy in enumerate(copies):
            got(copy)
            total = total + sums[which, i + 1, :, cols]
        return lax.rsqrt(total / features + epsilon)

    def place():
        experts = 128
        e_id = lax.broadcasted_iota(jnp.int32, (experts, n_tok), 0).astype(F32)
        named = jnp.zeros((experts, n_tok), F32)
        for k in range(4):
            named += (e_id == meta_in[k : k + 1]).astype(F32)
        before = (
            lax.broadcasted_iota(jnp.int32, (n_tok, n_tok), 0)
            < lax.broadcasted_iota(jnp.int32, (n_tok, n_tok), 1)
        )
        counts = jnp.dot(
            named.astype(BF), before.astype(F32).astype(BF), preferred_element_type=F32
        )
        for k in range(4):
            route = meta_in[k : k + 1]
            slot = jnp.sum(jnp.where(e_id == route, counts, 0.0), axis=0, keepdims=True)
            meta[0, k : k + 1] = route * CAP + slot
        meta[0, 4:8] = meta_in[4:8]

    far = nz // 2
    z_meta, z_inv, z_data = {}, {}, {}

    def send_block(direction, d, h):
        step = 1 if direction == 0 else -1
        src, dst = ((nz - d + 1) % nz, nz - d) if direction == 0 else (d - 1, d)
        part_rows = pl.ds(h * half, half)
        z_data[direction, d, h] = push(
            blocks.at[src, part_rows], blocks.at[dst, part_rows], device(dz=step)
        )

    def send_small(kept, array, direction, d):
        step = 1 if direction == 0 else -1
        src, dst = ((nz - d + 1) % nz, nz - d) if direction == 0 else (d - 1, d)
        kept[direction, d] = push(array.at[src], array.at[dst], device(dz=step))

    token_load.wait()
    pl.semaphore_wait(barrier, len(peers))
    for h in range(2):
        for direction in range(2):
            send_block(direction, 1, h)
    values = blocks[0].astype(F32)
    all_tokens = pl.ds(0, n_tok)
    norm_copies = start_norm(values, 0, all_tokens)
    place()
    for direction in range(2):
        send_small(z_meta, meta, direction, 1)
    inv[0] = end_norm(norm_copies, 0, all_tokens)
    for direction in range(2):
        send_small(z_inv, inv, direction, 1)

    def normalized(r):
        values = blocks[r].astype(F32)
        return (values * spread(inv[r], values.shape[1]) * gain[...]).astype(BF)

    normed[...] = normalized(0)

    x_copies, ret_copies, flight = {}, {}, {}

    def slot_ids(shape):
        s = lax.broadcasted_iota(jnp.int32, shape, 0)
        per = 4 * CAP
        return (z * (NX * per) + (x + s // per) % NX * per + s % per).astype(F32)

    def phase_a(i):
        if i == 0:
            return
        for direction in range(2):
            for kept, array in ((z_meta, meta), (z_inv, inv)):
                if (direction, i) in kept:
                    got(kept[direction, i])
                    if i + 1 < far or (i + 1 == far and direction == 0):
                        send_small(kept, array, direction, i + 1)
        for h in range(2):
            for direction in range(2):
                if (direction, i, h) in z_data:
                    got(z_data[direction, i, h])
                    if i + 1 < far or (i + 1 == far and h == direction):
                        send_block(direction, i + 1, h)

    def phase_b(i):
        for r in STAGES[i]:
            ids = slot_ids((n_tok, n_tok))
            pick = jnp.zeros((n_tok, n_tok), F32)
            for k in range(4):
                pick = jnp.where(ids == meta[r, k : k + 1], 1.0, pick)
            rows = jnp.dot(
                pick.astype(BF),
                normed[...] if r == 0 else normalized(r),
                preferred_element_type=F32,
            ).astype(BF)
            rows = rows.reshape(NX, 4, CAP, rows.shape[-1])
            rows_in[r, 0] = rows[0]
            for dx in range(1, NX):
                rows_out[r, dx] = rows[dx]
            x_copies[r] = [
                push(rows_out.at[r, dx], rows_in.at[r, dx], device(dx=dx)) for dx in range(1, NX)
            ]

    def span(i):
        n = 64 * (1 if i == SHARED else len(STAGES[i]))
        return pl.ds(OFFSET[i], n), n

    def phase_c(i):
        rows, n = span(i)
        need("shared")
        if i != SHARED:
            need("up")
            for r in STAGES[i]:
                for copy in x_copies[r]:
                    got(copy)

        def one(dy, carry):
            e = (y + dy) % ny
            w = 4 if i == SHARED else e
            taken = []
            for core in (1 - c, c):
                if i == SHARED:
                    taken.append(normed[pl.ds(pl.multiple_of((e * 2 + core) * 64, 64), 64)])
                else:
                    for r in STAGES[i]:
                        for k in range(2):
                            taken.append(rows_in[r, core * 2 + k, e])
            left = jnp.concatenate(taken, axis=0)
            for at, weights in ((0, wg), (1, wu)):
                got = jnp.dot(left, weights[w], preferred_element_type=F32).astype(BF)
                cols = pl.ds(at * 512, 512)
                for_partner[dy, rows, cols] = got[:n]
                own_part[dy, rows, cols] = got[n:]
            return carry

        lax.fori_loop(0, ny, one, 0)
        flight["d", i] = push(
            for_partner.at[:, rows], from_partner.at[:, rows], device(dc=1)
        )

    def phase_d(i):
        rows, n = span(i)
        got(flight["d", i])
        flight["y", i] = []
        for dy in range(1, ny):
            own_part[dy, rows] = (
                own_part[dy, rows].astype(F32) + from_partner[dy, rows].astype(F32)
            ).astype(BF)
            flight["y", i].append(
                push(own_part.at[dy, rows], from_y.at[dy - 1, rows], device(dy=dy))
            )

    def phase_e(i):
        rows, n = span(i)
        for copy in flight["y", i]:
            got(copy)
        pre = own_part[0, rows].astype(F32) + from_partner[0, rows].astype(F32)
        for dy in range(1, ny):
            pre = pre + from_y[dy - 1, rows].astype(F32)
        gate, up = pre[:, :512], pre[:, 512:]
        hid[0, 0, rows] = (gate / (1.0 + jnp.exp(-gate)) * up).astype(BF)
        flight["h", i] = [
            push(hid.at[0, 0, rows], hid.at[0, ny - dy, rows], device(dy=dy))
            for dy in range(1, ny)
        ]

    def phase_f(i):
        rows, n = span(i)
        for copy in flight["h", i]:
            got(copy)
        flight["g", i] = push(hid.at[0, :, rows], hid.at[1, :, rows], device(dc=1))

    def phase_g(i):
        rows, n = span(i)
        need("down")
        got(flight["g", i])
        if i != SHARED:
            for r in STAGES[i]:
                sent(x_copies[r])

        def one(dy, carry):
            e = (y + dy) % ny
            w = 4 if i == SHARED else e
            left = jnp.concatenate([hid[0, dy, rows], hid[1, dy, rows]], axis=0)
            got = jnp.dot(left, wd[w], preferred_element_type=F32).astype(BF)
            for at, core in ((0, c), (n, 1 - c)):
                if i == SHARED:
                    shared_out[pl.ds(pl.multiple_of((e * 2 + core) * 64, 64), 64)] = got[
                        at : at + n
                    ]
                else:
                    for j, r in enumerate(STAGES[i]):
                        for k in range(2):
                            first = at + j * 64 + k * CAP
                            rows_out[r, core * 2 + k, e] = got[first : first + CAP]
            return carry

        lax.fori_loop(0, ny, one, 0)
        if i != SHARED:
            for r in STAGES[i]:
                ret_copies[r] = [
                    push(rows_out.at[r, dx], returned.at[r, dx - 1], device(dx=-dx))
                    for dx in range(1, NX)
                ]

    def combine(r):
        for copy in ret_copies[r]:
            got(copy)
        ids = slot_ids((n_tok, n_tok))
        weight = jnp.zeros((n_tok, n_tok), F32)
        for k in range(4):
            weight = jnp.where(ids == meta[r, k : k + 1], meta[r, 4 + k : 5 + k], weight)
        expert_rows = jnp.concatenate(
            [rows_out[r, 0].reshape(4 * CAP, -1), returned[r].reshape(3 * 4 * CAP, -1)], axis=0
        )
        return lax.dot_general(
            weight.astype(BF), expert_rows, (((0,), (0,)), ((), ())), preferred_element_type=F32
        )

    z_sum = {}
    z_slot = {(0, 1): 0, (1, 1): 1, (0, 2): 2, (1, 2): 3, (0, 3): 4, (1, 3): 5, (0, 0): 6, (1, 0): 7}

    def send_sum(direction, r, h):
        d = (r if direction == 0 else nz - r) - 1
        rows = pl.ds(h * half, half)
        z_sum[direction, d, h] = push(
            blocks.at[r, rows], z_in.at[z_slot[direction, d], rows],
            device(dz=1 if direction == 0 else -1),
        )

    def phase_z(d):
        if d == far:
            total = combine(far)
            blocks[far] = total.astype(BF)
            send_sum(0, far, 0)
            send_sum(1, far, 1)
            return
        if d > 0:
            for direction, r in ((0, d), (1, nz - d)):
                part[direction] = combine(r)
            for h in range(2):
                rows = pl.ds(h * half, half)
                for direction, r in ((0, d), (1, nz - d)):
                    total = part[direction, rows]
                    if (direction, d, h) in z_sum:
                        got(z_sum[direction, d, h])
                        total = total + z_in[z_slot[direction, d], rows].astype(F32)
                    for key in [k for k in z_data if source_of(k) == (r, h)]:
                        sent([z_data.pop(key)])
                    blocks[r, rows] = total.astype(BF)
                    send_sum(direction, r, h)
            return
        part[0] = combine(0) + shared_out[...].astype(F32)
        copies = []
        for h in range(2):
            rows = pl.ds(h * half, half)
            total = part[0, rows]
            for direction in range(2):
                got(z_sum[direction, 0, h])
                total = total + z_in[z_slot[direction, 0], rows].astype(F32)
            mix[rows] = total
            copies.append(start_norm(total, 1, rows))
        for h in range(2):
            rows = pl.ds(h * half, half)
            inverse = spread(end_norm(copies[h], 1, rows), mix.shape[1])
            out_ref[rows] = (mix[rows] * inverse * post[...]).astype(BF)

    def source_of(key):
        direction, d, h = key
        return ((nz - d + 1) % nz if direction == 0 else d - 1, h)

    phases = dict(
        A=phase_a, B=phase_b, C=phase_c, D=phase_d, E=phase_e, F=phase_f, G=phase_g, Z=phase_z
    )
    for item in schedule:
        phases[item[0]](int(item[1]))

    sent(list(sends.values()))
    for copy in list(awaited.values()):
        got(copy)
    for name in list(weight_loads):
        need(name)


def per_device(mesh_shape, schedule, tokens, routes, route_weights, pre_gain, eg, eu, ed, sg, su, sd, post_gain):
    n_tok, width = tokens.shape
    nz, ny = mesh_shape["ep"] // NX, mesh_shape["tp"] // NC
    meta = jnp.concatenate([routes.T.astype(F32), route_weights.T], axis=0)
    local = eg.shape[0]
    hidden = eg.shape[2]
    vmem = pl.BlockSpec(memory_space=pltpu.VMEM)
    hbm = pl.BlockSpec(memory_space=pl.ANY)
    nsem = 200
    return pl.pallas_call(
        functools.partial(kernel, nz, ny, width * mesh_shape["tp"], schedule),
        out_shape=jax.ShapeDtypeStruct((n_tok, width), BF),
        in_specs=[hbm, vmem, vmem, vmem] + [hbm] * 6,
        out_specs=vmem,
        scratch_shapes=[
            pltpu.VMEM((n_tok, width), BF),
            pltpu.VMEM((local + 1, width, hidden), BF),
            pltpu.VMEM((local + 1, width, hidden), BF),
            pltpu.VMEM((local + 1, hidden, width), BF),
            pltpu.VMEM((nz, n_tok, width), BF),
            pltpu.VMEM((nz, 8, n_tok), F32),
            pltpu.VMEM((nz, 1, n_tok), F32),
            pltpu.VMEM((nz, NX, local, CAP, width), BF),
            pltpu.VMEM((nz, NX, local, CAP, width), BF),
            pltpu.VMEM((ny, ROWS, 2 * hidden), BF),
            pltpu.VMEM((ny, ROWS, 2 * hidden), BF),
            pltpu.VMEM((ny, ROWS, 2 * hidden), BF),
            pltpu.VMEM((ny - 1, ROWS, 2 * hidden), BF),
            pltpu.VMEM((2, ny, ROWS, hidden), BF),
            pltpu.VMEM((nz, NX - 1, local, CAP, width), BF),
            pltpu.VMEM((n_tok, width), BF),
            pltpu.VMEM((8, n_tok, width), BF),
            pltpu.VMEM((2, n_tok, width), F32),
            pltpu.VMEM((n_tok, width), F32),
            pltpu.VMEM((2, 8, 1, n_tok), F32),
            pltpu.SemaphoreType.DMA((nsem,)),
            pltpu.SemaphoreType.DMA((nsem,)),
            pltpu.SemaphoreType.DMA((8,)),
        ],
        compiler_params=pltpu.CompilerParams(
            collective_id=0, has_side_effects=True, vmem_limit_bytes=66_000_000
        ),
        name="layer",
    )(tokens, meta, pre_gain[None, :], post_gain[None, :], eg, eu, ed, sg, su, sd)


def solution(mesh, schedule=None):
    in_specs = (
        P("ep", "tp"),
        P("ep", None),
        P("ep", None),
        P("tp"),
        P("ep", "tp", None),
        P("ep", "tp", None),
        P("ep", None, "tp"),
        P("tp", None),
        P("tp", None),
        P(None, "tp"),
        P("tp"),
    )
    return jax.shard_map(
        functools.partial(per_device, dict(mesh.shape), tuple(schedule or SCHEDULE)),
        mesh=mesh,
        in_specs=in_specs,
        out_specs=P("ep", "tp"),
        check_vma=False,
    )
```

```python
import functools

import jax
import jax.numpy as jnp
from jax import lax
from jax.experimental import pallas as pl
from jax.experimental.pallas import tpu as pltpu
from jax.sharding import PartitionSpec as P

MESH = pl.DeviceIdType.MESH
BF, F32 = jnp.bfloat16, jnp.float32
epsilon = 1e-06

NX, NC = 4, 2
CAP = 32

SHARED = 8
UNIT = 64
ROWS = UNIT * (SHARED + 1)

SCHEDULE = " ".join(
    (
        "A0 C8 B0 D8",
        "A1 a1 B7 C0",
        "A2 B1 D0 E8",
        "a2 B6 B2 C7",
        "A3 D7 C6 D6",
        "a3 B3 C1 C2",
        "D2 A4 a4 B4",
        "C3 E6 D3 C4",
        "B5 D4 E3 E4",
        "C5 D5 F3 G3",
        "F4 G4 E5 E2",
        "F5 D1 G5 F6",
        "F2 Z4 G2 E1",
        "E0 G6 Z3 F1",
        "E7 G1 z3 F7",
        "G7 F8 Z2 z2",
        "Z1 G8 F0 G0",
        "z1 Z0 z0",
    )
).split()


def kernel(
    nz,
    ny,
    features,
    schedule,
    tok_hbm,
    routes,
    route_weights,
    gain,
    post,
    wg_hbm,
    wu_hbm,
    wd_hbm,
    sg_hbm,
    su_hbm,
    sd_hbm,
    out_ref,
    normed,
    wg,
    wu,
    wd,
    blocks,
    meta,
    inv,
    rows_out,
    rows_in,
    own_part,
    for_partner,
    from_partner,
    from_y,
    hid,
    returned,
    shared_out,
    z_in,
    part,
    sums,
    send_sem,
    recv_sem,
    local_sem,
):
    ep, tp = lax.axis_index("ep"), lax.axis_index("tp")
    z, x = ep // NX, ep % NX
    y, c = tp // NC, tp % NC
    n_tok = normed.shape[0]
    half = n_tok // 2

    def device(dz=0, dx=0, dy=0, dc=0):
        return (
            (z + dz + nz) % nz * NX + (x + dx + NX) % NX,
            (y + dy + ny) % ny * NC + (c + dc) % NC,
        )

    used = [0, 0]
    sends, awaited = {}, {}

    def push(src, dst, to):
        i = used[0]
        used[0] += 1
        copy = pltpu.make_async_remote_copy(
            src_ref=src,
            dst_ref=dst,
            send_sem=send_sem.at[i],
            recv_sem=recv_sem.at[i],
            device_id=to,
            device_id_type=MESH,
        )
        copy.start()
        sends[id(copy)] = copy
        awaited[id(copy)] = copy
        return copy

    def got(copy):
        awaited.pop(id(copy)).wait_recv()

    def sent(copies):
        for copy in copies:
            sends.pop(id(copy)).wait_send()

    def load(src, dst):
        copy = pltpu.make_async_copy(src, dst, local_sem.at[used[1]])
        used[1] += 1
        copy.start()
        return copy

    token_load = load(tok_hbm, blocks.at[0])
    weight_loads = {
        "shared": [load(sg_hbm, wg.at[4]), load(su_hbm, wu.at[4])],
        "up": [load(wg_hbm, wg.at[pl.ds(0, 4)]), load(wu_hbm, wu.at[pl.ds(0, 4)])],
        "down": [load(sd_hbm, wd.at[4]), load(wd_hbm, wd.at[pl.ds(0, 4)])],
    }

    def need(name):
        for copy in weight_loads.pop(name, []):
            copy.wait()

    peers = [device(dz=1), device(dz=-1)]
    peers += [device(dx=dx) for dx in range(1, NX)]
    tp_steps = [(dy, dc) for dy in range(ny) for dc in range(NC)][1:]
    peers += [device(dy=dy, dc=dc) for dy, dc in tp_steps]
    barrier = pltpu.get_barrier_semaphore()
    for peer in peers:
        pl.semaphore_signal(barrier, inc=1, device_id=peer, device_id_type=MESH)

    def to_row(column):
        n = column.shape[0]
        same = lax.broadcasted_iota(jnp.int32, (n, n), 0) == lax.broadcasted_iota(
            jnp.int32, (n, n), 1
        )
        return jnp.sum(jnp.where(same, column, 0.0), axis=0, keepdims=True)

    def spread(row, width):
        high = row.astype(BF)
        rest = row - high.astype(F32)
        middle = rest.astype(BF)
        low = (rest - middle.astype(F32)).astype(BF)
        left = jnp.concatenate([high, middle, low, jnp.zeros((13, row.shape[1]), BF)], axis=0)
        column = lax.dot_general(
            left, jnp.ones((16, 128), BF), (((0,), (0,)), ((), ())), preferred_element_type=F32
        )
        return jnp.concatenate([column] * (width // 128), axis=1)

    def start_norm(values, which, cols):
        sums[which, 0, :, cols] = to_row(jnp.sum(values * values, axis=1, keepdims=True))
        return [
            push(
                sums.at[which, 0, :, cols],
                sums.at[which, i + 1, :, cols],
                device(dy=dy, dc=dc),
            )
            for i, (dy, dc) in enumerate(tp_steps)
        ]

    def end_norm(copies, which, cols):
        total = sums[which, 0, :, cols]
        for i, copy in enumerate(copies):
            got(copy)
            total = total + sums[which, i + 1, :, cols]
        return lax.rsqrt(total / features + epsilon)

    def place():
        experts = 128
        e_id = lax.broadcasted_iota(jnp.int32, (experts, n_tok), 0).astype(F32)
        named = jnp.zeros((experts, n_tok), F32)
        for k in range(4):
            named += (e_id == routes[k : k + 1].astype(F32)).astype(F32)
        before = (
            lax.broadcasted_iota(jnp.int32, (n_tok, n_tok), 0)
            < lax.broadcasted_iota(jnp.int32, (n_tok, n_tok), 1)
        )
        counts = jnp.dot(
            named.astype(BF), before.astype(F32).astype(BF), preferred_element_type=F32
        )
        for k in range(4):
            route = routes[k : k + 1].astype(F32)
            slot = jnp.sum(jnp.where(e_id == route, counts, 0.0), axis=0, keepdims=True)
            meta[0, k : k + 1] = route * CAP + slot
        meta[0, 4:8] = route_weights[...]

    far = nz // 2
    z_meta, z_inv, z_data = {}, {}, {}

    def send_block(direction, d, h):
        step = 1 if direction == 0 else -1
        src, dst = ((nz - d + 1) % nz, nz - d) if direction == 0 else (d - 1, d)
        part_rows = pl.ds(h * half, half)
        z_data[direction, d, h] = push(
            blocks.at[src, part_rows], blocks.at[dst, part_rows], device(dz=step)
        )

    def send_small(kept, array, direction, d):
        step = 1 if direction == 0 else -1
        src, dst = ((nz - d + 1) % nz, nz - d) if direction == 0 else (d - 1, d)
        kept[direction, d] = push(array.at[src], array.at[dst], device(dz=step))

    token_load.wait()
    pl.semaphore_wait(barrier, len(peers))
    for h in range(2):
        for direction in range(2):
            send_block(direction, 1, h)
    values = blocks[0].astype(F32)
    all_tokens = pl.ds(0, n_tok)
    norm_copies = start_norm(values, 0, all_tokens)
    place()
    for direction in range(2):
        send_small(z_meta, meta, direction, 1)
    inv[0] = end_norm(norm_copies, 0, all_tokens)
    for direction in range(2):
        send_small(z_inv, inv, direction, 1)

    def normalized(r):
        values = blocks[r].astype(F32)
        return (values * spread(inv[r], values.shape[1]) * gain[...]).astype(BF)

    normed[...] = normalized(0)

    x_copies, ret_copies, flight = {}, {}, {}

    def slot_ids(shape):
        s = lax.broadcasted_iota(jnp.int32, shape, 0)
        per = 4 * CAP
        return (z * (NX * per) + (x + s // per) % NX * per + s % per).astype(F32)

    def phase_a(d, h):
        if d == 0:
            return
        if h == 0:
            for direction in range(2):
                for kept, array in ((z_meta, meta), (z_inv, inv)):
                    if (direction, d) in kept:
                        got(kept[direction, d])
                        if d + 1 < far or (d + 1 == far and direction == 0):
                            send_small(kept, array, direction, d + 1)
        for direction in range(2):
            if (direction, d, h) in z_data:
                got(z_data[direction, d, h])
                if d + 1 < far or (d + 1 == far and h == direction):
                    send_block(direction, d + 1, h)

    def phase_b(r):
        ids = slot_ids((n_tok, n_tok))
        pick = jnp.zeros((n_tok, n_tok), F32)
        for k in range(4):
            pick = jnp.where(ids == meta[r, k : k + 1], 1.0, pick)
        rows = jnp.dot(
            pick.astype(BF),
            normed[...] if r == 0 else normalized(r),
            preferred_element_type=F32,
        ).astype(BF)
        rows = rows.reshape(NX, 4, CAP, rows.shape[-1])
        rows_in[r, 0] = rows[0]
        for dx in range(1, NX):
            rows_out[r, dx] = rows[dx]
        x_copies[r] = [
            push(rows_out.at[r, dx], rows_in.at[r, dx], device(dx=dx)) for dx in range(1, NX)
        ]

    def phase_c(i):
        rows = pl.ds(UNIT * i, UNIT)
        need("shared")
        if i != SHARED:
            need("up")
            for copy in x_copies[i]:
                got(copy)

        def one(dy, carry):
            e = (y + dy) % ny
            w = 4 if i == SHARED else e
            taken = []
            for core in (1 - c, c):
                if i == SHARED:
                    first = pl.multiple_of((e * 2 + core) * UNIT, UNIT)
                    taken.append(normed[pl.ds(first, UNIT)])
                else:
                    taken += [rows_in[i, core * 2 + k, e] for k in range(2)]
            left = jnp.concatenate(taken, axis=0)
            for at, weights in ((0, wg), (1, wu)):
                got_rows = jnp.dot(left, weights[w], preferred_element_type=F32).astype(BF)
                cols = pl.ds(at * 512, 512)
                for_partner[dy, rows, cols] = got_rows[:UNIT]
                own_part[dy, rows, cols] = got_rows[UNIT:]
            return carry

        lax.fori_loop(0, ny, one, 0)
        flight["d", i] = push(
            for_partner.at[:, rows], from_partner.at[:, rows], device(dc=1)
        )

    def phase_d(i):
        rows = pl.ds(UNIT * i, UNIT)
        got(flight["d", i])
        flight["y", i] = []
        for dy in range(1, ny):
            own_part[dy, rows] = (
                own_part[dy, rows].astype(F32) + from_partner[dy, rows].astype(F32)
            ).astype(BF)
            flight["y", i].append(
                push(own_part.at[dy, rows], from_y.at[dy - 1, rows], device(dy=dy))
            )

    def phase_e(i):
        rows = pl.ds(UNIT * i, UNIT)
        for copy in flight["y", i]:
            got(copy)
        pre = own_part[0, rows].astype(F32) + from_partner[0, rows].astype(F32)
        for dy in range(1, ny):
            pre = pre + from_y[dy - 1, rows].astype(F32)
        gate, up = pre[:, :512], pre[:, 512:]
        hid[0, 0, rows] = (gate / (1.0 + jnp.exp(-gate)) * up).astype(BF)
        flight["h", i] = [
            push(hid.at[0, 0, rows], hid.at[0, ny - dy, rows], device(dy=dy))
            for dy in range(1, ny)
        ]

    def phase_f(i):
        rows = pl.ds(UNIT * i, UNIT)
        for copy in flight["h", i]:
            got(copy)
        flight["g", i] = push(hid.at[0, :, rows], hid.at[1, :, rows], device(dc=1))

    def phase_g(i):
        rows = pl.ds(UNIT * i, UNIT)
        need("down")
        got(flight["g", i])
        if i != SHARED:
            sent(x_copies[i])

        def one(dy, carry):
            e = (y + dy) % ny
            w = 4 if i == SHARED else e
            left = jnp.concatenate([hid[0, dy, rows], hid[1, dy, rows]], axis=0)
            out = jnp.dot(left, wd[w], preferred_element_type=F32).astype(BF)
            for at, core in ((0, c), (UNIT, 1 - c)):
                if i == SHARED:
                    first = pl.multiple_of((e * 2 + core) * UNIT, UNIT)
                    shared_out[pl.ds(first, UNIT)] = out[at : at + UNIT]
                else:
                    for k in range(2):
                        first = at + k * CAP
                        rows_out[i, core * 2 + k, e] = out[first : first + CAP]
            return carry

        lax.fori_loop(0, ny, one, 0)
        if i != SHARED:
            ret_copies[i] = [
                push(rows_out.at[i, dx], returned.at[i, dx - 1], device(dx=-dx))
                for dx in range(1, NX)
            ]

    def combine(r):
        for copy in ret_copies[r]:
            got(copy)
        ids = slot_ids((n_tok, n_tok))
        weight = jnp.zeros((n_tok, n_tok), F32)
        for k in range(4):
            weight = jnp.where(ids == meta[r, k : k + 1], meta[r, 4 + k : 5 + k], weight)
        expert_rows = jnp.concatenate(
            [rows_out[r, 0].reshape(4 * CAP, -1), returned[r].reshape(3 * 4 * CAP, -1)], axis=0
        )
        return lax.dot_general(
            weight.astype(BF), expert_rows, (((0,), (0,)), ((), ())), preferred_element_type=F32
        )

    z_sum = {}
    z_slot = {(0, 1): 0, (1, 1): 1, (0, 2): 2, (1, 2): 3, (0, 3): 4, (1, 3): 5, (0, 0): 6, (1, 0): 7}

    def send_sum(direction, r, h):
        d = (r if direction == 0 else nz - r) - 1
        rows = pl.ds(h * half, half)
        z_sum[direction, d, h] = push(
            blocks.at[r, rows], z_in.at[z_slot[direction, d], rows],
            device(dz=1 if direction == 0 else -1),
        )

    def ways(d):
        return ((0, d, 2 * (d % 2)), (1, (nz - d) % nz, 2 * (d % 2) + 1))

    def phase_z(d, h):
        rows = pl.ds(h * half, half)
        if d == far:
            total = combine(far)
            blocks[far] = total.astype(BF)
            send_sum(0, far, 0)
            send_sum(1, far, 1)
            return
        if h == 0:
            if d > 0:
                for direction, r, slot in ways(d):
                    part[slot] = combine(r)
            else:
                part[0] = combine(0) + shared_out[...].astype(F32)
        if d > 0:
            for direction, r, slot in ways(d):
                total = part[slot, rows]
                if (direction, d, h) in z_sum:
                    got(z_sum[direction, d, h])
                    total = total + z_in[z_slot[direction, d], rows].astype(F32)
                for key in [k for k in z_data if source_of(k) == (r, h)]:
                    sent([z_data.pop(key)])
                blocks[r, rows] = total.astype(BF)
                send_sum(direction, r, h)
            return
        total = part[0, rows]
        for direction in range(2):
            got(z_sum[direction, 0, h])
            total = total + z_in[z_slot[direction, 0], rows].astype(F32)
        part[0, rows] = total
        flight["n", h] = start_norm(total, 1, rows)
        if h == 1:
            for k in range(2):
                rows = pl.ds(k * half, half)
                inverse = spread(end_norm(flight["n", k], 1, rows), part.shape[2])
                out_ref[rows] = (part[0, rows] * inverse * post[...]).astype(BF)

    def source_of(key):
        direction, d, h = key
        return ((nz - d + 1) % nz if direction == 0 else d - 1, h)

    phases = dict(B=phase_b, C=phase_c, D=phase_d, E=phase_e, F=phase_f, G=phase_g)
    halves = dict(A=(phase_a, 0), a=(phase_a, 1), Z=(phase_z, 0), z=(phase_z, 1))
    for item in schedule:
        if item[0] in phases:
            phases[item[0]](int(item[1]))
        else:
            phase, h = halves[item[0]]
            phase(int(item[1]), h)

    sent(list(sends.values()))
    for copy in list(awaited.values()):
        got(copy)
    for name in list(weight_loads):
        need(name)


def per_device(mesh_shape, schedule, tokens, routes, route_weights, pre_gain, eg, eu, ed, sg, su, sd, post_gain):
    n_tok, width = tokens.shape
    nz, ny = mesh_shape["ep"] // NX, mesh_shape["tp"] // NC
    local = eg.shape[0]
    hidden = eg.shape[2]
    vmem = pl.BlockSpec(memory_space=pltpu.VMEM)
    hbm = pl.BlockSpec(memory_space=pl.ANY)
    nsem = 240
    return pl.pallas_call(
        functools.partial(kernel, nz, ny, width * mesh_shape["tp"], schedule),
        out_shape=jax.ShapeDtypeStruct((n_tok, width), BF),
        in_specs=[hbm] + [vmem] * 4 + [hbm] * 6,
        out_specs=vmem,
        scratch_shapes=[
            pltpu.VMEM((n_tok, width), BF),
            pltpu.VMEM((local + 1, width, hidden), BF),
            pltpu.VMEM((local + 1, width, hidden), BF),
            pltpu.VMEM((local + 1, hidden, width), BF),
            pltpu.VMEM((nz, n_tok, width), BF),
            pltpu.VMEM((nz, 8, n_tok), F32),
            pltpu.VMEM((nz, 1, n_tok), F32),
            pltpu.VMEM((nz, NX, local, CAP, width), BF),
            pltpu.VMEM((nz, NX, local, CAP, width), BF),
            pltpu.VMEM((ny, ROWS, 2 * hidden), BF),
            pltpu.VMEM((ny, ROWS, 2 * hidden), BF),
            pltpu.VMEM((ny, ROWS, 2 * hidden), BF),
            pltpu.VMEM((ny - 1, ROWS, 2 * hidden), BF),
            pltpu.VMEM((2, ny, ROWS, hidden), BF),
            pltpu.VMEM((nz, NX - 1, local, CAP, width), BF),
            pltpu.VMEM((n_tok, width), BF),
            pltpu.VMEM((8, n_tok, width), BF),
            pltpu.VMEM((4, n_tok, width), F32),
            pltpu.VMEM((2, 8, 1, n_tok), F32),
            pltpu.SemaphoreType.DMA((nsem,)),
            pltpu.SemaphoreType.DMA((nsem,)),
            pltpu.SemaphoreType.DMA((8,)),
        ],
        compiler_params=pltpu.CompilerParams(
            collective_id=0, has_side_effects=True, vmem_limit_bytes=66_000_000
        ),
        name="layer",
    )(
        tokens,
        routes.T,
        route_weights.T,
        pre_gain[None, :],
        post_gain[None, :],
        eg,
        eu,
        ed,
        sg,
        su,
        sd,
    )


def solution(mesh, schedule=None):
    in_specs = (
        P("ep", "tp"),
        P("ep", None),
        P("ep", None),
        P("tp"),
        P("ep", "tp", None),
        P("ep", "tp", None),
        P("ep", None, "tp"),
        P("tp", None),
        P("tp", None),
        P(None, "tp"),
        P("tp"),
    )
    return jax.shard_map(
        functools.partial(per_device, dict(mesh.shape), tuple(schedule or SCHEDULE)),
        mesh=mesh,
        in_specs=in_specs,
        out_specs=P("ep", "tp"),
        check_vma=False,
    )
```

```python
import functools

import jax
import jax.numpy as jnp
from jax import lax
from jax.experimental import pallas as pl
from jax.experimental.pallas import tpu as pltpu
from jax.sharding import PartitionSpec as P

MESH = pl.DeviceIdType.MESH
BF, F32 = jnp.bfloat16, jnp.float32
epsilon = 1e-06

NX, NC = 4, 2
CAP = 32

SHARED = 8
UNIT = 64
ROWS = UNIT * (SHARED + 1)

SCHEDULE = " ".join(
    (
        "A0 C8 B0 D8",
        "A1 a1 B7 C0",
        "A2 B1 D0 E8",
        "a2 B6 B2 C7",
        "A3 D7 C6 D6",
        "a3 B3 C1 C2",
        "D2 A4 a4 B4",
        "C3 D3 C4 B5",
        "D4 E3 E4 C5",
        "D5 E6 F3 G3",
        "F4 G4 E5 E2",
        "F5 D1 G5 F6",
        "F2 Z4 G2 E1",
        "E0 G6 Z3 F1",
        "E7 G1 z3 F7",
        "G7 F8 Z2 z2",
        "Z1 G8 F0 G0",
        "z1 Z0 z0",
    )
).split()


def kernel(
    nz,
    ny,
    features,
    schedule,
    tok_hbm,
    routes,
    route_weights,
    gain,
    wg_hbm,
    wu_hbm,
    wd_hbm,
    sg_hbm,
    su_hbm,
    sd_hbm,
    out_ref,
    normed,
    wg,
    wu,
    wd,
    blocks,
    meta,
    inv,
    rows_out,
    rows_in,
    own_part,
    for_partner,
    from_partner,
    from_y,
    hid,
    returned,
    shared_out,
    z_in,
    part,
    sums,
    send_sem,
    recv_sem,
    local_sem,
):
    ep, tp = lax.axis_index("ep"), lax.axis_index("tp")
    z, x = ep // NX, ep % NX
    y, c = tp // NC, tp % NC
    n_tok = normed.shape[0]
    half = n_tok // 2

    def device(dz=0, dx=0, dy=0, dc=0):
        return (
            (z + dz + nz) % nz * NX + (x + dx + NX) % NX,
            (y + dy + ny) % ny * NC + (c + dc) % NC,
        )

    def far_first(n):
        return sorted(range(1, n), key=lambda k: -min(k, n - k))

    used = [0, 0]
    sends, awaited = {}, {}

    def push(src, dst, to):
        i = used[0]
        used[0] += 1
        copy = pltpu.make_async_remote_copy(
            src_ref=src,
            dst_ref=dst,
            send_sem=send_sem.at[i],
            recv_sem=recv_sem.at[i],
            device_id=to,
            device_id_type=MESH,
        )
        copy.start()
        sends[id(copy)] = copy
        awaited[id(copy)] = copy
        return copy

    def got(copy):
        awaited.pop(id(copy)).wait_recv()

    def sent(copies):
        for copy in copies:
            sends.pop(id(copy)).wait_send()

    def load(src, dst):
        copy = pltpu.make_async_copy(src, dst, local_sem.at[used[1]])
        used[1] += 1
        copy.start()
        return copy

    token_load = load(tok_hbm, blocks.at[0])
    weight_loads = {
        "shared": [load(sg_hbm, wg.at[4]), load(su_hbm, wu.at[4])],
        "up": [load(wg_hbm, wg.at[pl.ds(0, 4)]), load(wu_hbm, wu.at[pl.ds(0, 4)])],
        "down": [load(sd_hbm, wd.at[4]), load(wd_hbm, wd.at[pl.ds(0, 4)])],
    }

    def need(name):
        for copy in weight_loads.pop(name, []):
            copy.wait()

    peers = [device(dz=1), device(dz=-1)]
    peers += [device(dx=dx) for dx in range(1, NX)]
    tp_steps = [(dy, dc) for dy in range(ny) for dc in range(NC)][1:]
    peers += [device(dy=dy, dc=dc) for dy, dc in tp_steps]
    barrier = pltpu.get_barrier_semaphore()
    for peer in peers:
        pl.semaphore_signal(barrier, inc=1, device_id=peer, device_id_type=MESH)

    def to_row(column):
        n = column.shape[0]
        same = lax.broadcasted_iota(jnp.int32, (n, n), 0) == lax.broadcasted_iota(
            jnp.int32, (n, n), 1
        )
        return jnp.sum(jnp.where(same, column, 0.0), axis=0, keepdims=True)

    def spread(row, width):
        high = row.astype(BF)
        rest = row - high.astype(F32)
        middle = rest.astype(BF)
        low = (rest - middle.astype(F32)).astype(BF)
        left = jnp.concatenate([high, middle, low, jnp.zeros((13, row.shape[1]), BF)], axis=0)
        column = lax.dot_general(
            left, jnp.ones((16, 128), BF), (((0,), (0,)), ((), ())), preferred_element_type=F32
        )
        return jnp.concatenate([column] * (width // 128), axis=1)

    def start_norm(values, which, cols):
        sums[which, 0, :, cols] = to_row(jnp.sum(values * values, axis=1, keepdims=True))
        return [
            push(
                sums.at[which, 0, :, cols],
                sums.at[which, i + 1, :, cols],
                device(dy=dy, dc=dc),
            )
            for i, (dy, dc) in enumerate(tp_steps)
        ]

    def end_norm(copies, which, cols):
        total = sums[which, 0, :, cols]
        for i, copy in enumerate(copies):
            got(copy)
            total = total + sums[which, i + 1, :, cols]
        return lax.rsqrt(total / features + epsilon)

    def place():
        experts = 128
        e_id = lax.broadcasted_iota(jnp.int32, (experts, n_tok), 0).astype(F32)
        named = jnp.zeros((experts, n_tok), F32)
        for k in range(4):
            named += (e_id == routes[k : k + 1].astype(F32)).astype(F32)
        before = (
            lax.broadcasted_iota(jnp.int32, (n_tok, n_tok), 0)
            < lax.broadcasted_iota(jnp.int32, (n_tok, n_tok), 1)
        )
        counts = jnp.dot(
            named.astype(BF), before.astype(F32).astype(BF), preferred_element_type=F32
        )
        for k in range(4):
            route = routes[k : k + 1].astype(F32)
            slot = jnp.sum(jnp.where(e_id == route, counts, 0.0), axis=0, keepdims=True)
            meta[0, k : k + 1] = route * CAP + slot
        meta[0, 4:8] = route_weights[...]

    far = nz // 2
    z_meta, z_inv, z_data = {}, {}, {}

    def send_block(direction, d, h):
        step = 1 if direction == 0 else -1
        src, dst = ((nz - d + 1) % nz, nz - d) if direction == 0 else (d - 1, d)
        part_rows = pl.ds(h * half, half)
        z_data[direction, d, h] = push(
            blocks.at[src, part_rows], blocks.at[dst, part_rows], device(dz=step)
        )

    def send_small(kept, array, direction, d):
        step = 1 if direction == 0 else -1
        src, dst = ((nz - d + 1) % nz, nz - d) if direction == 0 else (d - 1, d)
        kept[direction, d] = push(array.at[src], array.at[dst], device(dz=step))

    token_load.wait()
    pl.semaphore_wait(barrier, len(peers))
    for direction, h in ((0, 0), (1, 1), (0, 1), (1, 0)):
        send_block(direction, 1, h)
    values = blocks[0].astype(F32)
    all_tokens = pl.ds(0, n_tok)
    norm_copies = start_norm(values, 0, all_tokens)
    place()
    for direction in range(2):
        send_small(z_meta, meta, direction, 1)
    inv[0] = end_norm(norm_copies, 0, all_tokens)
    for direction in range(2):
        send_small(z_inv, inv, direction, 1)

    def normalized(r):
        values = blocks[r].astype(F32)
        return (values * spread(inv[r], values.shape[1]) * gain[...]).astype(BF)

    normed[...] = normalized(0)

    x_copies, ret_copies, flight = {}, {}, {}

    def slot_ids(shape):
        s = lax.broadcasted_iota(jnp.int32, shape, 0)
        per = 4 * CAP
        return (z * (NX * per) + (x + s // per) % NX * per + s % per).astype(F32)

    def phase_a(d, second):
        if d == 0:
            return
        if second == 0:
            for direction in range(2):
                for kept, array in ((z_meta, meta), (z_inv, inv)):
                    if (direction, d) in kept:
                        got(kept[direction, d])
                        if d + 1 < far or (d + 1 == far and direction == 0):
                            send_small(kept, array, direction, d + 1)
        for direction in range(2):
            h = direction if second == 0 else 1 - direction
            if (direction, d, h) in z_data:
                got(z_data[direction, d, h])
                if d + 1 < far or (d + 1 == far and h == direction):
                    send_block(direction, d + 1, h)

    def phase_b(r):
        ids = slot_ids((n_tok, n_tok))
        pick = jnp.zeros((n_tok, n_tok), F32)
        for k in range(4):
            pick = jnp.where(ids == meta[r, k : k + 1], 1.0, pick)
        rows = jnp.dot(
            pick.astype(BF),
            normed[...] if r == 0 else normalized(r),
            preferred_element_type=F32,
        ).astype(BF)
        rows = rows.reshape(NX, 4, CAP, rows.shape[-1])
        rows_in[r, 0] = rows[0]
        for dx in range(1, NX):
            rows_out[r, dx] = rows[dx]
        x_copies[r] = [
            push(rows_out.at[r, dx], rows_in.at[r, dx], device(dx=dx)) for dx in far_first(NX)
        ]

    def phase_c(i):
        rows = pl.ds(UNIT * i, UNIT)
        need("shared")
        if i != SHARED:
            need("up")
            for copy in x_copies[i]:
                got(copy)

        def one(dy, carry):
            e = (y + dy) % ny
            w = 4 if i == SHARED else e
            taken = []
            for core in (1 - c, c):
                if i == SHARED:
                    first = pl.multiple_of((e * 2 + core) * UNIT, UNIT)
                    taken.append(normed[pl.ds(first, UNIT)])
                else:
                    taken += [rows_in[i, core * 2 + k, e] for k in range(2)]
            left = jnp.concatenate(taken, axis=0)
            for at, weights in ((0, wg), (1, wu)):
                got_rows = jnp.dot(left, weights[w], preferred_element_type=F32).astype(BF)
                cols = pl.ds(at * 512, 512)
                for_partner[dy, rows, cols] = got_rows[:UNIT]
                own_part[dy, rows, cols] = got_rows[UNIT:]
            return carry

        lax.fori_loop(0, ny, one, 0, unroll=True)
        flight["d", i] = push(
            for_partner.at[:, rows], from_partner.at[:, rows], device(dc=1)
        )

    def phase_d(i):
        rows = pl.ds(UNIT * i, UNIT)
        got(flight["d", i])
        flight["y", i] = []
        for dy in far_first(ny):
            own_part[dy, rows] = (
                own_part[dy, rows].astype(F32) + from_partner[dy, rows].astype(F32)
            ).astype(BF)
            flight["y", i].append(
                push(own_part.at[dy, rows], from_y.at[dy - 1, rows], device(dy=dy))
            )

    def phase_e(i):
        rows = pl.ds(UNIT * i, UNIT)
        for copy in flight["y", i]:
            got(copy)
        pre = own_part[0, rows].astype(F32) + from_partner[0, rows].astype(F32)
        for dy in range(1, ny):
            pre = pre + from_y[dy - 1, rows].astype(F32)
        gate, up = pre[:, :512], pre[:, 512:]
        hid[0, 0, rows] = (gate / (1.0 + jnp.exp(-gate)) * up).astype(BF)
        flight["h", i] = [
            push(hid.at[0, 0, rows], hid.at[0, ny - dy, rows], device(dy=dy))
            for dy in far_first(ny)
        ]

    def phase_f(i):
        rows = pl.ds(UNIT * i, UNIT)
        for copy in flight["h", i]:
            got(copy)
        flight["g", i] = push(hid.at[0, :, rows], hid.at[1, :, rows], device(dc=1))

    def phase_g(i):
        rows = pl.ds(UNIT * i, UNIT)
        need("down")
        got(flight["g", i])
        if i != SHARED:
            sent(x_copies[i])

        def one(dy, carry):
            e = (y + dy) % ny
            w = 4 if i == SHARED else e
            left = jnp.concatenate([hid[0, dy, rows], hid[1, dy, rows]], axis=0)
            out = jnp.dot(left, wd[w], preferred_element_type=F32).astype(BF)
            for at, core in ((0, c), (UNIT, 1 - c)):
                if i == SHARED:
                    first = pl.multiple_of((e * 2 + core) * UNIT, UNIT)
                    shared_out[pl.ds(first, UNIT)] = out[at : at + UNIT]
                else:
                    for k in range(2):
                        first = at + k * CAP
                        rows_out[i, core * 2 + k, e] = out[first : first + CAP]
            return carry

        lax.fori_loop(0, ny, one, 0, unroll=True)
        if i != SHARED:
            ret_copies[i] = [
                push(rows_out.at[i, dx], returned.at[i, dx - 1], device(dx=-dx))
                for dx in far_first(NX)
            ]

    def combine(r):
        for copy in ret_copies[r]:
            got(copy)
        ids = slot_ids((n_tok, n_tok))
        weight = jnp.zeros((n_tok, n_tok), F32)
        for k in range(4):
            weight = jnp.where(ids == meta[r, k : k + 1], meta[r, 4 + k : 5 + k], weight)
        expert_rows = jnp.concatenate(
            [rows_out[r, 0].reshape(4 * CAP, -1), returned[r].reshape(3 * 4 * CAP, -1)], axis=0
        )
        return lax.dot_general(
            weight.astype(BF), expert_rows, (((0,), (0,)), ((), ())), preferred_element_type=F32
        )

    z_sum = {}
    z_slot = {(0, 1): 0, (1, 1): 1, (0, 2): 2, (1, 2): 3, (0, 3): 4, (1, 3): 5, (0, 0): 6, (1, 0): 7}

    def send_sum(direction, r, h):
        d = (r if direction == 0 else nz - r) - 1
        rows = pl.ds(h * half, half)
        z_sum[direction, d, h] = push(
            blocks.at[r, rows], z_in.at[z_slot[direction, d], rows],
            device(dz=1 if direction == 0 else -1),
        )

    def ways(d):
        return ((0, d, 2 * (d % 2)), (1, (nz - d) % nz, 2 * (d % 2) + 1))

    def phase_z(d, second):
        if d == far:
            total = combine(far)
            blocks[far] = total.astype(BF)
            send_sum(0, far, 0)
            send_sum(1, far, 1)
            return
        if second == 0:
            if d > 0:
                for direction, r, slot in ways(d):
                    part[slot] = combine(r)
            else:
                part[0] = combine(0) + shared_out[...].astype(F32)
        if d > 0:
            for direction, r, slot in ways(d):
                h = second if direction == 1 else 1 - second
                rows = pl.ds(h * half, half)
                total = part[slot, rows]
                if (direction, d, h) in z_sum:
                    got(z_sum[direction, d, h])
                    total = total + z_in[z_slot[direction, d], rows].astype(F32)
                for key in [k for k in z_data if source_of(k) == (r, h)]:
                    sent([z_data.pop(key)])
                blocks[r, rows] = total.astype(BF)
                send_sum(direction, r, h)
            return
        if second == 0:
            return
        for h in range(2):
            rows = pl.ds(h * half, half)
            total = part[0, rows]
            for direction in (1 - h, h):
                got(z_sum[direction, 0, h])
                total = total + z_in[z_slot[direction, 0], rows].astype(F32)
            part[0, rows] = total
            flight["n", h] = start_norm(total, 1, rows)
        for h in range(2):
            finish(h)

    def finish(h):
        rows = pl.ds(h * half, half)
        inverse = spread(end_norm(flight["n", h], 1, rows), part.shape[2])
        part[1, rows] = part[0, rows] * inverse
        flight["out", h] = load(part.at[1, rows], out_ref.at[rows])

    def source_of(key):
        direction, d, h = key
        return ((nz - d + 1) % nz if direction == 0 else d - 1, h)

    phases = dict(B=phase_b, C=phase_c, D=phase_d, E=phase_e, F=phase_f, G=phase_g)
    halves = dict(A=(phase_a, 0), a=(phase_a, 1), Z=(phase_z, 0), z=(phase_z, 1))
    for item in schedule:
        if item[0] in phases:
            phases[item[0]](int(item[1]))
        else:
            phase, h = halves[item[0]]
            phase(int(item[1]), h)

    sent(list(sends.values()))
    for h in range(2):
        if ("out", h) in flight:
            flight["out", h].wait()
    for copy in list(awaited.values()):
        got(copy)
    for name in list(weight_loads):
        need(name)


def per_device(mesh_shape, schedule, tokens, routes, route_weights, pre_gain, eg, eu, ed, sg, su, sd, post_gain):
    n_tok, width = tokens.shape
    nz, ny = mesh_shape["ep"] // NX, mesh_shape["tp"] // NC
    local = eg.shape[0]
    hidden = eg.shape[2]
    vmem = pl.BlockSpec(memory_space=pltpu.VMEM)
    hbm = pl.BlockSpec(memory_space=pl.ANY)
    nsem = 240
    scaled = pl.pallas_call(
        functools.partial(kernel, nz, ny, width * mesh_shape["tp"], schedule),
        out_shape=jax.ShapeDtypeStruct((n_tok, width), F32),
        in_specs=[hbm] + [vmem] * 3 + [hbm] * 6,
        out_specs=hbm,
        scratch_shapes=[
            pltpu.VMEM((n_tok, width), BF),
            pltpu.VMEM((local + 1, width, hidden), BF),
            pltpu.VMEM((local + 1, width, hidden), BF),
            pltpu.VMEM((local + 1, hidden, width), BF),
            pltpu.VMEM((nz, n_tok, width), BF),
            pltpu.VMEM((nz, 8, n_tok), F32),
            pltpu.VMEM((nz, 1, n_tok), F32),
            pltpu.VMEM((nz, NX, local, CAP, width), BF),
            pltpu.VMEM((nz, NX, local, CAP, width), BF),
            pltpu.VMEM((ny, ROWS, 2 * hidden), BF),
            pltpu.VMEM((ny, ROWS, 2 * hidden), BF),
            pltpu.VMEM((ny, ROWS, 2 * hidden), BF),
            pltpu.VMEM((ny - 1, ROWS, 2 * hidden), BF),
            pltpu.VMEM((2, ny, ROWS, hidden), BF),
            pltpu.VMEM((nz, NX - 1, local, CAP, width), BF),
            pltpu.VMEM((n_tok, width), BF),
            pltpu.VMEM((8, n_tok, width), BF),
            pltpu.VMEM((4, n_tok, width), F32),
            pltpu.VMEM((2, 8, 1, n_tok), F32),
            pltpu.SemaphoreType.DMA((nsem,)),
            pltpu.SemaphoreType.DMA((nsem,)),
            pltpu.SemaphoreType.DMA((12,)),
        ],
        compiler_params=pltpu.CompilerParams(
            collective_id=0, has_side_effects=True, vmem_limit_bytes=66_000_000
        ),
        name="layer",
    )(
        tokens,
        routes.T,
        route_weights.T,
        pre_gain[None, :],
        eg,
        eu,
        ed,
        sg,
        su,
        sd,
    )
    return (scaled * post_gain[None, :]).astype(BF)


def solution(mesh, schedule=None):
    in_specs = (
        P("ep", "tp"),
        P("ep", None),
        P("ep", None),
        P("tp"),
        P("ep", "tp", None),
        P("ep", "tp", None),
        P("ep", None, "tp"),
        P("tp", None),
        P("tp", None),
        P(None, "tp"),
        P("tp"),
    )
    return jax.shard_map(
        functools.partial(per_device, dict(mesh.shape), tuple(schedule or SCHEDULE)),
        mesh=mesh,
        in_specs=in_specs,
        out_specs=P("ep", "tp"),
        check_vma=False,
    )
```

```python
import functools

import jax
import jax.numpy as jnp
from jax import lax
from jax.experimental import pallas as pl
from jax.experimental.pallas import tpu as pltpu
from jax.sharding import PartitionSpec as P

MESH = pl.DeviceIdType.MESH
BF, F32 = jnp.bfloat16, jnp.float32
epsilon = 1e-06

NX, NC = 4, 2
CAP = 32

SHARED = 8
UNIT = 64
ROWS = UNIT * (SHARED + 1)

SCHEDULE = " ".join(
    (
        "A0 C8 B0 D8",
        "A1 a1 B7 C0",
        "A2 B1 D0 E8",
        "a2 B6 B2 C7",
        "A3 D7 C6 D6",
        "a3 B3 C1 C2",
        "D2 A4 a4 B4",
        "C3 D3 C4 B5",
        "D4 E3 E4 C5",
        "D5 E6 F3 G3",
        "F4 G4 E5 E2",
        "F5 D1 G5 F6",
        "F2 Z4 G2 E1",
        "E0 G6 Z3 F1",
        "E7 G1 z3 F7",
        "G7 F8 Z2 z2",
        "Z1 G8 F0 G0",
        "z1 Z0 z0",
    )
).split()


def kernel(
    nz,
    ny,
    features,
    schedule,
    tok_hbm,
    routes,
    route_weights,
    gain,
    wg_hbm,
    wu_hbm,
    wd_hbm,
    sg_hbm,
    su_hbm,
    sd_hbm,
    out_ref,
    normed,
    wg,
    wu,
    wd,
    blocks,
    meta,
    inv,
    rows_out,
    rows_in,
    own_part,
    for_partner,
    from_partner,
    from_y,
    hid,
    returned,
    shared_out,
    z_in,
    part,
    sums,
    send_sem,
    recv_sem,
    local_sem,
):
    ep, tp = lax.axis_index("ep"), lax.axis_index("tp")
    z, x = ep // NX, ep % NX
    y, c = tp // NC, tp % NC
    n_tok = normed.shape[0]
    half = n_tok // 2

    def device(dz=0, dx=0, dy=0, dc=0):
        return (
            (z + dz + nz) % nz * NX + (x + dx + NX) % NX,
            (y + dy + ny) % ny * NC + (c + dc) % NC,
        )

    def far_first(n):
        return sorted(range(1, n), key=lambda k: -min(k, n - k))

    used = [0, 0]
    sends, awaited = {}, {}

    def push(src, dst, to):
        i = used[0]
        used[0] += 1
        copy = pltpu.make_async_remote_copy(
            src_ref=src,
            dst_ref=dst,
            send_sem=send_sem.at[i],
            recv_sem=recv_sem.at[i],
            device_id=to,
            device_id_type=MESH,
        )
        copy.start()
        sends[id(copy)] = copy
        awaited[id(copy)] = copy
        return copy

    def got(copy):
        awaited.pop(id(copy)).wait_recv()

    def sent(copies):
        for copy in copies:
            sends.pop(id(copy)).wait_send()

    def load(src, dst):
        copy = pltpu.make_async_copy(src, dst, local_sem.at[used[1]])
        used[1] += 1
        copy.start()
        return copy

    token_load = load(tok_hbm, blocks.at[0])
    weight_loads = {
        "shared": [load(sg_hbm, wg.at[4]), load(su_hbm, wu.at[4])],
        "up": [load(wg_hbm, wg.at[pl.ds(0, 4)]), load(wu_hbm, wu.at[pl.ds(0, 4)])],
        "down": [load(sd_hbm, wd.at[4]), load(wd_hbm, wd.at[pl.ds(0, 4)])],
    }

    def need(name):
        for copy in weight_loads.pop(name, []):
            copy.wait()

    peers = [device(dz=1), device(dz=-1)]
    peers += [device(dx=dx) for dx in range(1, NX)]
    tp_steps = [(dy, dc) for dy in range(ny) for dc in range(NC)][1:]
    peers += [device(dy=dy, dc=dc) for dy, dc in tp_steps]
    barrier = pltpu.get_barrier_semaphore()
    for peer in peers:
        pl.semaphore_signal(barrier, inc=1, device_id=peer, device_id_type=MESH)

    def to_row(column):
        n = column.shape[0]
        same = lax.broadcasted_iota(jnp.int32, (n, n), 0) == lax.broadcasted_iota(
            jnp.int32, (n, n), 1
        )
        return jnp.sum(jnp.where(same, column, 0.0), axis=0, keepdims=True)

    def spread(row, width):
        high = row.astype(BF)
        rest = row - high.astype(F32)
        middle = rest.astype(BF)
        low = (rest - middle.astype(F32)).astype(BF)
        left = jnp.concatenate([high, middle, low, jnp.zeros((13, row.shape[1]), BF)], axis=0)
        column = lax.dot_general(
            left, jnp.ones((16, 128), BF), (((0,), (0,)), ((), ())), preferred_element_type=F32
        )
        return jnp.concatenate([column] * (width // 128), axis=1)

    def start_norm(values, which, cols):
        sums[which, 0, :, cols] = to_row(jnp.sum(values * values, axis=1, keepdims=True))
        return [
            push(
                sums.at[which, 0, :, cols],
                sums.at[which, i + 1, :, cols],
                device(dy=dy, dc=dc),
            )
            for i, (dy, dc) in enumerate(tp_steps)
        ]

    def end_norm(copies, which, cols):
        total = sums[which, 0, :, cols]
        for i, copy in enumerate(copies):
            got(copy)
            total = total + sums[which, i + 1, :, cols]
        return lax.rsqrt(total / features + epsilon)

    def place():
        experts = 128
        e_id = lax.broadcasted_iota(jnp.int32, (experts, n_tok), 0).astype(F32)
        named = jnp.zeros((experts, n_tok), F32)
        for k in range(4):
            named += (e_id == routes[k : k + 1].astype(F32)).astype(F32)
        before = (
            lax.broadcasted_iota(jnp.int32, (n_tok, n_tok), 0)
            < lax.broadcasted_iota(jnp.int32, (n_tok, n_tok), 1)
        )
        counts = jnp.dot(
            named.astype(BF), before.astype(F32).astype(BF), preferred_element_type=F32
        )
        for k in range(4):
            route = routes[k : k + 1].astype(F32)
            slot = jnp.sum(jnp.where(e_id == route, counts, 0.0), axis=0, keepdims=True)
            meta[0, k : k + 1] = route * CAP + slot
        meta[0, 4:8] = route_weights[...]

    far = nz // 2
    z_meta, z_inv, z_data = {}, {}, {}

    def send_block(direction, d, h):
        step = 1 if direction == 0 else -1
        src, dst = ((nz - d + 1) % nz, nz - d) if direction == 0 else (d - 1, d)
        part_rows = pl.ds(h * half, half)
        z_data[direction, d, h] = push(
            blocks.at[src, part_rows], blocks.at[dst, part_rows], device(dz=step)
        )

    def send_small(kept, array, direction, d):
        step = 1 if direction == 0 else -1
        src, dst = ((nz - d + 1) % nz, nz - d) if direction == 0 else (d - 1, d)
        kept[direction, d] = push(array.at[src], array.at[dst], device(dz=step))

    token_load.wait()
    pl.semaphore_wait(barrier, len(peers))
    for direction, h in ((0, 0), (1, 1), (0, 1), (1, 0)):
        send_block(direction, 1, h)
    values = blocks[0].astype(F32)
    all_tokens = pl.ds(0, n_tok)
    norm_copies = start_norm(values, 0, all_tokens)
    place()
    for direction in range(2):
        send_small(z_meta, meta, direction, 1)
    inv[0] = end_norm(norm_copies, 0, all_tokens)
    for direction in range(2):
        send_small(z_inv, inv, direction, 1)

    def normalized(r):
        values = blocks[r].astype(F32)
        return (values * spread(inv[r], values.shape[1]) * gain[...]).astype(BF)

    normed[...] = normalized(0)

    x_copies, ret_copies, flight = {}, {}, {}

    def slot_ids(shape):
        s = lax.broadcasted_iota(jnp.int32, shape, 0)
        per = 4 * CAP
        return (z * (NX * per) + (x + s // per) % NX * per + s % per).astype(F32)

    def phase_a(d, second):
        if d == 0:
            return
        if second == 0:
            for direction in range(2):
                for kept, array in ((z_meta, meta), (z_inv, inv)):
                    if (direction, d) in kept:
                        got(kept[direction, d])
                        if d + 1 < far or (d + 1 == far and direction == 0):
                            send_small(kept, array, direction, d + 1)
        for direction in range(2):
            h = direction if second == 0 else 1 - direction
            if (direction, d, h) in z_data:
                got(z_data[direction, d, h])
                if d + 1 < far or (d + 1 == far and h == direction):
                    send_block(direction, d + 1, h)

    def phase_b(r):
        ids = slot_ids((n_tok, n_tok))
        pick = jnp.zeros((n_tok, n_tok), F32)
        for k in range(4):
            pick = jnp.where(ids == meta[r, k : k + 1], 1.0, pick)
        rows = jnp.dot(
            pick.astype(BF),
            normed[...] if r == 0 else normalized(r),
            preferred_element_type=F32,
        ).astype(BF)
        rows = rows.reshape(NX, 4, CAP, rows.shape[-1])
        rows_in[r, 0] = rows[0]
        for dx in range(1, NX):
            rows_out[r, dx] = rows[dx]
        x_copies[r] = [
            push(rows_out.at[r, dx], rows_in.at[r, dx], device(dx=dx)) for dx in far_first(NX)
        ]

    def phase_c(i):
        rows = pl.ds(UNIT * i, UNIT)
        need("shared")
        if i != SHARED:
            need("up")
            for copy in x_copies[i]:
                got(copy)

        def one(dy, carry):
            e = (y + dy) % ny
            w = 4 if i == SHARED else e
            taken = []
            for core in (1 - c, c):
                if i == SHARED:
                    first = pl.multiple_of((e * 2 + core) * UNIT, UNIT)
                    taken.append(normed[pl.ds(first, UNIT)])
                else:
                    taken += [rows_in[i, core * 2 + k, e] for k in range(2)]
            left = jnp.concatenate(taken, axis=0)
            for at, weights in ((0, wg), (1, wu)):
                got_rows = jnp.dot(left, weights[w], preferred_element_type=F32).astype(BF)
                cols = pl.ds(at * 512, 512)
                for_partner[dy, rows, cols] = got_rows[:UNIT]
                own_part[dy, rows, cols] = got_rows[UNIT:]
            return carry

        lax.fori_loop(0, ny, one, 0, unroll=True)
        flight["d", i] = push(
            for_partner.at[:, rows], from_partner.at[:, rows], device(dc=1)
        )

    def phase_d(i):
        rows = pl.ds(UNIT * i, UNIT)
        got(flight["d", i])
        flight["y", i] = []
        for dy in far_first(ny):
            own_part[dy, rows] = (
                own_part[dy, rows].astype(F32) + from_partner[dy, rows].astype(F32)
            ).astype(BF)
            flight["y", i].append(
                push(own_part.at[dy, rows], from_y.at[dy - 1, rows], device(dy=dy))
            )

    def phase_e(i):
        rows = pl.ds(UNIT * i, UNIT)
        for copy in flight["y", i]:
            got(copy)
        pre = own_part[0, rows].astype(F32) + from_partner[0, rows].astype(F32)
        for dy in range(1, ny):
            pre = pre + from_y[dy - 1, rows].astype(F32)
        gate, up = pre[:, :512], pre[:, 512:]
        hid[0, 0, rows] = (gate / (1.0 + jnp.exp(-gate)) * up).astype(BF)
        flight["h", i] = [
            push(hid.at[0, 0, rows], hid.at[0, ny - dy, rows], device(dy=dy))
            for dy in far_first(ny)
        ]

    def phase_f(i):
        rows = pl.ds(UNIT * i, UNIT)
        for copy in flight["h", i]:
            got(copy)
        flight["g", i] = push(hid.at[0, :, rows], hid.at[1, :, rows], device(dc=1))

    def phase_g(i):
        rows = pl.ds(UNIT * i, UNIT)
        need("down")
        got(flight["g", i])
        if i != SHARED:
            sent(x_copies[i])

        def one(dy, carry):
            e = (y + dy) % ny
            w = 4 if i == SHARED else e
            left = jnp.concatenate([hid[0, dy, rows], hid[1, dy, rows]], axis=0)
            out = jnp.dot(left, wd[w], preferred_element_type=F32).astype(BF)
            for at, core in ((0, c), (UNIT, 1 - c)):
                if i == SHARED:
                    first = pl.multiple_of((e * 2 + core) * UNIT, UNIT)
                    shared_out[pl.ds(first, UNIT)] = out[at : at + UNIT]
                else:
                    for k in range(2):
                        first = at + k * CAP
                        rows_out[i, core * 2 + k, e] = out[first : first + CAP]
            return carry

        lax.fori_loop(0, ny, one, 0, unroll=True)
        if i != SHARED:
            ret_copies[i] = [
                push(rows_out.at[i, dx], returned.at[i, dx - 1], device(dx=-dx))
                for dx in far_first(NX)
            ]

    def combine(r):
        for copy in ret_copies[r]:
            got(copy)
        ids = slot_ids((n_tok, n_tok))
        weight = jnp.zeros((n_tok, n_tok), F32)
        for k in range(4):
            weight = jnp.where(ids == meta[r, k : k + 1], meta[r, 4 + k : 5 + k], weight)
        expert_rows = jnp.concatenate(
            [rows_out[r, 0].reshape(4 * CAP, -1), returned[r].reshape(3 * 4 * CAP, -1)], axis=0
        )
        return lax.dot_general(
            weight.astype(BF), expert_rows, (((0,), (0,)), ((), ())), preferred_element_type=F32
        )

    z_sum = {}
    z_slot = {(0, 1): 0, (1, 1): 1, (0, 2): 2, (1, 2): 3, (0, 3): 4, (1, 3): 5, (0, 0): 6, (1, 0): 7}

    def send_sum(direction, r, h):
        d = (r if direction == 0 else nz - r) - 1
        rows = pl.ds(h * half, half)
        z_sum[direction, d, h] = push(
            blocks.at[r, rows], z_in.at[z_slot[direction, d], rows],
            device(dz=1 if direction == 0 else -1),
        )

    def ways(d):
        return ((0, d, 2 * (d % 2)), (1, (nz - d) % nz, 2 * (d % 2) + 1))

    def phase_z(d, second):
        if d == far:
            total = combine(far)
            blocks[far] = total.astype(BF)
            send_sum(0, far, 0)
            send_sum(1, far, 1)
            return
        if second == 0:
            if d > 0:
                for direction, r, slot in ways(d):
                    part[slot] = combine(r)
            else:
                part[0] = combine(0) + shared_out[...].astype(F32)
        if d > 0:
            for direction, r, slot in ways(d):
                h = second if direction == 1 else 1 - second
                rows = pl.ds(h * half, half)
                total = part[slot, rows]
                if (direction, d, h) in z_sum:
                    got(z_sum[direction, d, h])
                    total = total + z_in[z_slot[direction, d], rows].astype(F32)
                for key in [k for k in z_data if source_of(k) == (r, h)]:
                    sent([z_data.pop(key)])
                blocks[r, rows] = total.astype(BF)
                send_sum(direction, r, h)
            return
        if second == 0:
            for direction in range(2):
                h = 1 - direction
                rows = pl.ds(h * half, half)
                got(z_sum[direction, 0, h])
                part[0, rows] = part[0, rows] + z_in[z_slot[direction, 0], rows].astype(F32)
            return
        for h in range(2):
            rows = pl.ds(h * half, half)
            got(z_sum[h, 0, h])
            total = part[0, rows] + z_in[z_slot[h, 0], rows].astype(F32)
            part[0, rows] = total
            flight["n", h] = start_norm(total, 1, rows)
        for h in range(2):
            finish(h)

    def finish(h):
        rows = pl.ds(h * half, half)
        inverse = spread(end_norm(flight["n", h], 1, rows), part.shape[2])
        part[1, rows] = part[0, rows] * inverse
        flight["out", h] = load(part.at[1, rows], out_ref.at[rows])

    def source_of(key):
        direction, d, h = key
        return ((nz - d + 1) % nz if direction == 0 else d - 1, h)

    phases = dict(B=phase_b, C=phase_c, D=phase_d, E=phase_e, F=phase_f, G=phase_g)
    halves = dict(A=(phase_a, 0), a=(phase_a, 1), Z=(phase_z, 0), z=(phase_z, 1))
    for item in schedule:
        if item[0] in phases:
            phases[item[0]](int(item[1]))
        else:
            phase, h = halves[item[0]]
            phase(int(item[1]), h)

    sent(list(sends.values()))
    for h in range(2):
        if ("out", h) in flight:
            flight["out", h].wait()
    for copy in list(awaited.values()):
        got(copy)
    for name in list(weight_loads):
        need(name)


def per_device(mesh_shape, schedule, tokens, routes, route_weights, pre_gain, eg, eu, ed, sg, su, sd, post_gain):
    n_tok, width = tokens.shape
    nz, ny = mesh_shape["ep"] // NX, mesh_shape["tp"] // NC
    local = eg.shape[0]
    hidden = eg.shape[2]
    vmem = pl.BlockSpec(memory_space=pltpu.VMEM)
    hbm = pl.BlockSpec(memory_space=pl.ANY)
    nsem = 240
    scaled = pl.pallas_call(
        functools.partial(kernel, nz, ny, width * mesh_shape["tp"], schedule),
        out_shape=jax.ShapeDtypeStruct((n_tok, width), F32),
        in_specs=[hbm] + [vmem] * 3 + [hbm] * 6,
        out_specs=hbm,
        scratch_shapes=[
            pltpu.VMEM((n_tok, width), BF),
            pltpu.VMEM((local + 1, width, hidden), BF),
            pltpu.VMEM((local + 1, width, hidden), BF),
            pltpu.VMEM((local + 1, hidden, width), BF),
            pltpu.VMEM((nz, n_tok, width), BF),
            pltpu.VMEM((nz, 8, n_tok), F32),
            pltpu.VMEM((nz, 1, n_tok), F32),
            pltpu.VMEM((nz, NX, local, CAP, width), BF),
            pltpu.VMEM((nz, NX, local, CAP, width), BF),
            pltpu.VMEM((ny, ROWS, 2 * hidden), BF),
            pltpu.VMEM((ny, ROWS, 2 * hidden), BF),
            pltpu.VMEM((ny, ROWS, 2 * hidden), BF),
            pltpu.VMEM((ny - 1, ROWS, 2 * hidden), BF),
            pltpu.VMEM((2, ny, ROWS, hidden), BF),
            pltpu.VMEM((nz, NX - 1, local, CAP, width), BF),
            pltpu.VMEM((n_tok, width), BF),
            pltpu.VMEM((8, n_tok, width), BF),
            pltpu.VMEM((4, n_tok, width), F32),
            pltpu.VMEM((2, 8, 1, n_tok), F32),
            pltpu.SemaphoreType.DMA((nsem,)),
            pltpu.SemaphoreType.DMA((nsem,)),
            pltpu.SemaphoreType.DMA((12,)),
        ],
        compiler_params=pltpu.CompilerParams(
            collective_id=0, has_side_effects=True, vmem_limit_bytes=66_000_000
        ),
        name="layer",
    )(
        tokens,
        routes.T,
        route_weights.T,
        pre_gain[None, :],
        eg,
        eu,
        ed,
        sg,
        su,
        sd,
    )
    return (scaled * post_gain[None, :]).astype(BF)


def solution(mesh, schedule=None):
    in_specs = (
        P("ep", "tp"),
        P("ep", None),
        P("ep", None),
        P("tp"),
        P("ep", "tp", None),
        P("ep", "tp", None),
        P("ep", None, "tp"),
        P("tp", None),
        P("tp", None),
        P(None, "tp"),
        P("tp"),
    )
    return jax.shard_map(
        functools.partial(per_device, dict(mesh.shape), tuple(schedule or SCHEDULE)),
        mesh=mesh,
        in_specs=in_specs,
        out_specs=P("ep", "tp"),
        check_vma=False,
    )
```
